32 devices in a mesh: sp: 4 (over z), tp: 8 (over y, x, core).
Axes of the slice: x: 2, y: 2, z: 4, core: 2. Of those that a mesh axis runs over, the one named last changes fastest.
Arguments:
- context_activations: bfloat16 [2, 1024, 4096], P(None, 'sp', 'tp'), may hold values from -6 to 6
- first_generated_activation: bfloat16 [2, 4096], replicated, may hold values from -6 to 6
- address_projection: bfloat16 [4096, 1024], P(None, 'tp'), may hold values from -0.09375 to 0.09375
- payload_projection: bfloat16 [4096, 1024], P(None, 'tp'), may hold values from -0.09375 to 0.09375
- lookup_projection: bfloat16 [4096, 1024], P(None, 'tp'), may hold values from -0.09375 to 0.09375
- exit_gating_projection: bfloat16 [4096, 1024], P(None, 'tp'), may hold values from -0.09375 to 0.09375
- writing_intensity_projection: bfloat16 [4096, 8], replicated, may hold values from -0.09375 to 0.09375
- fading_projection: bfloat16 [4096, 8], replicated, may hold values from -0.09375 to 0.09375
- channel_fading_speed: float32 [8], replicated, may hold values from 0 to 1, as said below
- extra_fading_log: float32 [2, 1024, 8], P(None, 'sp', 'tp'), may hold values from -1 to 0, as said below
- readout_normalizer_gain: float32 [128], replicated, may hold values from 0.1 to 1.9
- exit_projection: bfloat16 [1024, 4096], P('tp'), may hold values from -0.1875 to 0.1875
Outputs:
- state_cache: bfloat16 [2, 4, 8, 128, 128], P(None, 'sp', 'tp')
- step_out: bfloat16 [2, 4096], P(None, 'tp')
The draws below stay inside these ranges and needn't reach their ends.
Inputs may be any that keep to these rules, and one draw needn't show every extreme that they name: `channel_fading_speed`: positive rates, one a head. `extra_fading_log`: zero at all but a few positions of each prompt and head, negative there.
All inputs are finite; a program needn't handle non-finite values.
Results may differ from the reference program's by a relative error of at most 0.012.
Values may be sent and summed in bfloat16 or wider, within the bound.
A program may use at most 64 MiB of HBM per device.

```python
import math
import jax
import jax.numpy as jnp
from jax import lax

D = 4096
HEAD = 128
BLOCK = 64
PROMPT_TOTAL = 2
SEG = 256
HEAD_TOTAL = 8
PROMPT_LENGTH = 1024


def draw_channel_fading_speed(key, part):
    pick_key, level_key = jax.random.split(jax.random.fold_in(key, 11))
    level = jax.random.uniform(level_key, (HEAD_TOTAL,), jnp.float32)
    slow_low = math.log(0.15 / (0.7 * PROMPT_LENGTH))
    slow_high = math.log(1.2 / (0.7 * PROMPT_LENGTH))
    slow_rate = jnp.exp(slow_low + level * (slow_high - slow_low))
    fast_low = math.log(1.0 / (0.7 * 50.0))
    fast_high = math.log(1.0 / (0.7 * 25.0))
    fast_rate = jnp.exp(fast_low + level * (fast_high - fast_low))
    which = jax.random.uniform(pick_key, (HEAD_TOTAL,), jnp.float32) < 0.5
    return jnp.where(which, fast_rate, slow_rate)


def draw_extra_fading_log(key, part):
    start_random_key, length_random_key = jax.random.split(jax.random.fold_in(key, 23))
    segment_start = jax.random.randint(start_random_key, (PROMPT_TOTAL, 1, HEAD_TOTAL, 2), 0, PROMPT_LENGTH)
    segment_length = jax.random.uniform(length_random_key, (PROMPT_TOTAL, 1, HEAD_TOTAL, 2), jnp.float32, -0.69, -0.22)
    split_places = jnp.arange(PROMPT_LENGTH)[None, :, None, None]
    return jnp.sum(jnp.where(split_places == segment_start, segment_length, 0.0), axis=-1)


def block_scale(own_key, dims, shards, smallest, top_value):
    loudness, own = 1.0, jax.random.fold_in(own_key, 6)
    for position, parts in shards:
        draws = jnp.exp(jax.random.uniform(jax.random.fold_in(own, position), (parts,), jnp.float32, smallest / len(shards), top_value / len(shards)))
        loudness = loudness * jnp.repeat(draws, dims[position] // parts).reshape([-1 if axis == position else 1 for axis in range(len(dims))])
    return loudness


def noise(stream_key, dims, deviation, limit, shards=(), kind=jnp.bfloat16):
    level = block_scale(stream_key, dims, shards, -0.22, 0.18) if shards else 1.0
    entries = jax.random.normal(stream_key, dims, jnp.float32) * deviation * level
    return jnp.minimum(jnp.maximum(entries, -limit), limit).astype(kind)


def setup_inputs(seed: int = 0) -> dict:
    keys = jax.random.split(jax.random.key(seed), 13)
    return {
        "context_activations": noise(keys[0], (PROMPT_TOTAL, PROMPT_LENGTH, D), 1.0, 6.0, ((1, 4), (2, 8))),
        "first_generated_activation": noise(keys[1], (PROMPT_TOTAL, D), 1.0, 6.0),
        "address_projection": noise(keys[2], (D, HEAD_TOTAL * HEAD), D ** -0.5, 0.09375, ((1, 8),)),
        "payload_projection": noise(keys[3], (D, HEAD_TOTAL * HEAD), D ** -0.5, 0.09375, ((1, 8),)),
        "lookup_projection": noise(keys[4], (D, HEAD_TOTAL * HEAD), D ** -0.5, 0.09375, ((1, 8),)),
        "exit_gating_projection": noise(keys[5], (D, HEAD_TOTAL * HEAD), D ** -0.5, 0.09375, ((1, 8),)),
        "writing_intensity_projection": noise(keys[6], (D, HEAD_TOTAL), D ** -0.5, 0.09375),
        "fading_projection": noise(keys[7], (D, HEAD_TOTAL), D ** -0.5, 0.09375),
        "channel_fading_speed": draw_channel_fading_speed(jax.random.fold_in(keys[12], 71), 0),
        "extra_fading_log": draw_extra_fading_log(jax.random.fold_in(keys[12], 71), 0),
        "readout_normalizer_gain": jnp.clip(1.0 + 0.18 * jax.random.normal(keys[10], (HEAD,), jnp.float32), 0.1, 1.9),
        "exit_projection": noise(keys[11], (HEAD_TOTAL * HEAD, D), (HEAD_TOTAL * HEAD) ** -0.5, 0.1875, ((0, 8),)),
    }


norm_eps = 1e-06
highest = lax.Precision.HIGHEST

def unit_rows(values_in):
    return values_in * lax.rsqrt(lax.optimization_barrier(jnp.sum(values_in * values_in, axis=-1, keepdims=True)) + norm_eps)

def boundary_states(keys_in, values_in, beta_gate, fading_exponent):
    blocks = keys_in.shape[0] // BLOCK
    key_blocks = keys_in.reshape(blocks, BLOCK, -1)
    value_blocks = values_in.reshape(blocks, BLOCK, -1)
    beta_blocks = beta_gate.reshape(blocks, BLOCK)
    cumul = jnp.cumsum(fading_exponent.reshape(blocks, BLOCK), axis=-1)
    causal = jnp.tril(jnp.ones((BLOCK, BLOCK), bool))
    strict = jnp.tril(jnp.ones((BLOCK, BLOCK), bool), -1)
    gaps_log = cumul[:, :, None] - cumul[:, None, :]
    within = jnp.where(causal, jnp.exp(jnp.where(causal, gaps_log, 0.0)), 0.0)
    keys_beta = key_blocks * beta_blocks[..., None]
    strict_part = jnp.where(strict, jnp.einsum('nid,njd->nij', keys_beta, key_blocks, precision=highest) * within, 0.0)
    targets = jnp.concatenate([value_blocks * beta_blocks[..., None], keys_beta * jnp.exp(cumul)[..., None]], axis=-1)
    system = jnp.eye(BLOCK, dtype=jnp.float32) + strict_part
    solved = lax.linalg.triangular_solve(system, targets, left_side=True, lower=True)
    width_v = value_blocks.shape[-1]
    pseudo_values = solved[..., :width_v]
    decayed_keys = solved[..., width_v:]
    trailing = key_blocks * jnp.exp(cumul[:, -1:] - cumul)[..., None]
    block_decay = jnp.exp(cumul[:, -1])

    def advance(memory, inputs):
        pseudo, decayed, trail_keys, shrink = inputs
        fresh_values = pseudo - jnp.dot(decayed, memory, precision=highest)
        memory = memory * shrink + jnp.dot(trail_keys.T, fresh_values, precision=highest)
        return (memory, memory)
    start_state = jnp.zeros((key_blocks.shape[-1], width_v), jnp.float32)
    _, every = lax.scan(advance, start_state, (pseudo_values, decayed_keys, trailing, block_decay))
    per_run = SEG // BLOCK
    return every[per_run - 1::per_run]

def one_sequence(inputs):
    keys_one, values_one, beta_one, decay_one = inputs
    return jax.vmap(boundary_states, in_axes=(1, 1, 1, 1), out_axes=1)(keys_one.astype(jnp.float32), values_one.astype(jnp.float32), beta_one, decay_one)

def reference(context_activations, first_generated_activation, address_projection, payload_projection, lookup_projection, exit_gating_projection, writing_intensity_projection, fading_projection, channel_fading_speed, extra_fading_log, readout_normalizer_gain, exit_projection):
    seq_count, length, width = context_activations.shape
    head_count = channel_fading_speed.shape[0]
    head_size = readout_normalizer_gain.shape[0]
    tokens = context_activations.reshape(seq_count * length, width)
    shaped = (seq_count, length, head_count, head_size)
    prompt_keys = unit_rows(jax.nn.silu(jnp.dot(tokens.astype(jnp.float32), address_projection.astype(jnp.float32), preferred_element_type=jnp.float32)).reshape(shaped)).astype(jnp.bfloat16)
    prompt_values = jax.nn.silu(jnp.dot(tokens.astype(jnp.float32), payload_projection.astype(jnp.float32), preferred_element_type=jnp.float32)).reshape(shaped).astype(jnp.bfloat16)
    beta_logit = jnp.dot(tokens.astype(jnp.float32), writing_intensity_projection.astype(jnp.float32), preferred_element_type=jnp.float32).astype(jnp.bfloat16).reshape(seq_count, length, head_count)
    fading_logit_entry = jnp.dot(tokens.astype(jnp.float32), fading_projection.astype(jnp.float32), preferred_element_type=jnp.float32).astype(jnp.bfloat16).reshape(seq_count, length, head_count)
    beta_gate = jax.nn.sigmoid(beta_logit.astype(jnp.float32))
    fading_exponent = extra_fading_log - channel_fading_speed * jax.nn.softplus(fading_logit_entry.astype(jnp.float32))
    runs = lax.map(one_sequence, (prompt_keys, prompt_values, beta_gate, fading_exponent))
    state_cache = runs.astype(jnp.bfloat16)
    states = runs[:, -1]
    heads_shape = (seq_count, head_count, head_size)
    new_keys = unit_rows(jax.nn.silu(jnp.dot(first_generated_activation.astype(jnp.float32), address_projection.astype(jnp.float32), preferred_element_type=jnp.float32)).reshape(heads_shape))
    new_values = jax.nn.silu(jnp.dot(first_generated_activation.astype(jnp.float32), payload_projection.astype(jnp.float32), preferred_element_type=jnp.float32)).reshape(heads_shape)
    new_queries = unit_rows(jax.nn.silu(jnp.dot(first_generated_activation.astype(jnp.float32), lookup_projection.astype(jnp.float32), preferred_element_type=jnp.float32)).reshape(heads_shape))
    out_gate = jax.nn.silu(jnp.dot(first_generated_activation.astype(jnp.float32), exit_gating_projection.astype(jnp.float32), preferred_element_type=jnp.float32)).reshape(heads_shape)
    new_beta = jax.nn.sigmoid(jnp.dot(first_generated_activation.astype(jnp.float32), writing_intensity_projection.astype(jnp.float32), preferred_element_type=jnp.float32))
    new_decay = jnp.exp(-channel_fading_speed * jax.nn.softplus(jnp.dot(first_generated_activation.astype(jnp.float32), fading_projection.astype(jnp.float32), preferred_element_type=jnp.float32)))
    recalled = jnp.einsum('shk,shkv->shv', new_keys, states, precision=highest)
    updated = new_decay[..., None, None] * (states - new_beta[..., None, None] * new_keys[..., None] * recalled[:, :, None, :])
    updated = updated + new_beta[..., None, None] * new_keys[..., None] * new_values[:, :, None, :]
    read = jnp.einsum('shk,shkv->shv', new_queries, updated, precision=highest)
    normed = read * lax.rsqrt(lax.optimization_barrier(jnp.mean(read * read, axis=-1, keepdims=True)) + norm_eps) * readout_normalizer_gain * out_gate
    normed = normed.astype(jnp.bfloat16).reshape(seq_count, head_count * head_size)
    step_out = jnp.dot(normed.astype(jnp.float32), exit_projection.astype(jnp.float32), preferred_element_type=jnp.float32).astype(jnp.bfloat16)
    return (state_cache, step_out)
```

```python
import functools

import jax
import jax.numpy as jnp
from jax import lax
from jax.experimental import pallas as pl
from jax.experimental.pallas import tpu as pltpu
from jax.sharding import PartitionSpec as P

EPS = 1e-06
BF = jnp.bfloat16
F32 = jnp.float32
MESH = pl.DeviceIdType.MESH


def mm(a, b, dims=((1,), (0,))):
    return lax.dot_general(a, b, (dims, ((), ())), preferred_element_type=F32)


def split(a):
    hi = a.astype(BF)
    return hi, (a - hi.astype(F32)).astype(BF)


def mm_split_left(a, b, dims=((1,), (0,))):
    hi, lo = split(a)
    return mm(hi, b, dims) + mm(lo, b, dims)


def mm_split_right(a, b):
    hi, lo = split(b)
    return mm(a, hi) + mm(a, lo)


def mm3(a, b):
    ah, al = split(a)
    bh, bl = split(b)
    return mm(ah, bh) + (mm(ah, bl) + mm(al, bh))


def silu(v):
    return v / (1.0 + jnp.exp(-v))


def sigmoid(v):
    return 1.0 / (1.0 + jnp.exp(-v))


def softplus(v):
    return jnp.maximum(v, 0.0) + jnp.log1p(jnp.exp(-jnp.abs(v)))


def unit(v):
    return v * lax.rsqrt(jnp.sum(v * v, axis=-1, keepdims=True) + EPS)


def to_col(row, eye):
    return jnp.sum(jnp.where(eye, row, 0.0), axis=1, keepdims=True)


def to_row(col, eye):
    return jnp.sum(jnp.where(eye, col, 0.0), axis=0, keepdims=True)


def local_maps(keys, values, beta, log_decay, extra):
    n = keys[0].shape[0]
    i = lax.broadcasted_iota(jnp.int32, (n, n), 0)
    j = lax.broadcasted_iota(jnp.int32, (n, n), 1)
    eye = i == j
    blocks = range(len(keys))
    rows, cols, systems, solved = [], [], [], []
    for b in blocks:
        fade = log_decay[b] + to_col(extra[b], eye)
        c_row = jnp.sum(jnp.where(i <= j, fade, 0.0), axis=0, keepdims=True)
        c_col = to_col(c_row, eye)
        gram = mm(keys[b], keys[b], ((1,), (1,)))
        within = jnp.exp(jnp.where(i > j, c_col - c_row, 0.0))
        systems.append(jnp.where(i > j, beta[b] * gram * within, 0.0))
        rows.append(c_row)
        cols.append(c_col)
    for b in blocks:
        solved.append(
            jnp.where(eye, 1.0, 0.0) - jnp.where((i // 2) == (j // 2), systems[b], 0.0)
        )
    size = 2
    while size < n:
        mask = ((i // (2 * size)) == (j // (2 * size))) & ((i // size) != (j // size))
        half = [mm3(jnp.where(mask, systems[b], 0.0), solved[b]) for b in blocks]
        solved = [solved[b] - mm3(solved[b], half[b]) for b in blocks]
        size *= 2
    total = None
    for b in blocks:
        beta_row = to_row(beta[b], eye)
        scaled = solved[b] * beta_row
        pseudo = mm_split_left(scaled, values[b])
        decayed = mm_split_left(scaled * jnp.exp(rows[b]), keys[b])
        last = cols[b][n - 1 : n, :]
        trail = jnp.exp(last - cols[b])
        both = jnp.concatenate([-decayed, pseudo], axis=1) * trail
        hi, lo = split(both)
        turned = ((0,), (0,))
        both = mm(keys[b], hi, turned) + mm(keys[b], lo, turned)
        width = keys[b].shape[1]
        wi = lax.broadcasted_iota(jnp.int32, (width, both.shape[1]), 0)
        wj = lax.broadcasted_iota(jnp.int32, (width, both.shape[1]), 1)
        both = both + jnp.where(wi == wj, jnp.exp(last), 0.0)
        if total is None:
            total = both
        else:
            width_off = jnp.where(wj >= width, both, 0.0)
            total = mm3(both[:, :width], total) + width_off
    return total


def kernel(
    n_sp,
    n_tp,
    block,
    ctx,
    first,
    wk_hbm,
    wv_hbm,
    wq_hbm,
    wz_hbm,
    wlog,
    speeds,
    extra,
    gain,
    exit_hbm,
    state_out,
    step_out,
    buf,
    wkv,
    wqz,
    wexit,
    acc,
    lacc,
    maps,
    prev,
    msg_out,
    msg_in,
    read_out,
    read_in,
    part,
    parts,
    local_sem,
    send_sem,
    recv_sem,
    chain_send,
    chain_recv,
    back_send,
    back_recv,
    read_send,
    read_recv,
    part_send,
    part_recv,
):
    prompts, length, feats = ctx.shape
    head = wk_hbm.shape[1]
    sp = lax.axis_index("sp")
    tp = lax.axis_index("tp")
    pairs = [(wk_hbm, wkv, 0), (wv_hbm, wkv, 1), (wq_hbm, wqz, 0), (wz_hbm, wqz, 1)]
    loads = [
        pltpu.make_async_copy(src, dst.at[:, pl.ds(at * head, head)], local_sem.at[k])
        for k, (src, dst, at) in enumerate(pairs)
    ]
    loads.append(pltpu.make_async_copy(exit_hbm, wexit, local_sem.at[4]))
    loads.append(pltpu.make_async_copy(ctx, buf.at[tp], local_sem.at[5]))
    loads[5].start()
    for copy in loads[:5]:
        copy.start()

    barrier = pltpu.get_barrier_semaphore()
    for d in range(1, n_tp):
        pl.semaphore_signal(
            barrier, inc=1, device_id=(sp, lax.rem(tp + d, n_tp)), device_id_type=MESH
        )
    for d in range(1, n_sp):
        pl.semaphore_signal(
            barrier, inc=1, device_id=(lax.rem(sp + d, n_sp), tp), device_id_type=MESH
        )
    pl.semaphore_wait(barrier, n_tp + n_sp - 2)

    def gather_copy(source, p, target, k, from_input=False):
        return pltpu.make_async_remote_copy(
            src_ref=ctx.at[p] if from_input else buf.at[source, p],
            dst_ref=buf.at[source, p],
            send_sem=send_sem.at[k, p],
            recv_sem=recv_sem.at[source, p],
            device_id=(sp, target),
            device_id_type=MESH,
        )

    sends = []

    def go(copy):
        copy.start()
        sends.append(copy)

    def arrived(source, p):
        gather_copy(source, p, tp, 0).wait_recv()

    cube = n_tp == 8
    if cube:
        y, x, core = tp // 4, (tp // 2) % 2, tp % 2

        def at(yy, xx, cc):
            return yy * 4 + xx * 2 + cc

        def turn(yy, xx, cc, first_axis):
            on_x = (1 - cc) if first_axis else cc
            on_y = cc if first_axis else (1 - cc)
            return yy + on_y * (1 - 2 * yy), xx + on_x * (1 - 2 * xx)

        near = at(*turn(y, x, core, True), core)
        far = at(*turn(y, x, core, False), core)
        across = at(1 - y, 1 - x, core)
        partner = at(y, x, 1 - core)
        near2 = at(*turn(y, x, 1 - core, True), 1 - core)
        far2 = at(*turn(y, x, 1 - core, False), 1 - core)
        across2 = at(1 - y, 1 - x, 1 - core)
        for p in range(prompts):
            go(gather_copy(tp, p, near, 0, True))
            go(gather_copy(tp, p, far, 1, True))
            go(gather_copy(tp, p, partner, 2, True))
    else:
        for p in range(prompts):
            for d in range(1, n_tp):
                go(gather_copy(tp, p, lax.rem(tp + d, n_tp), d, True))

    for copy in loads[:4]:
        copy.wait()
    x1 = first[...]
    kv1 = mm(x1, wkv[...])
    qz1 = mm(x1, wqz[...])
    l1 = mm(x1, wlog[...])
    k1 = unit(silu(kv1[:, :head]))
    v1 = silu(kv1[:, head:])
    q1 = unit(silu(qz1[:, :head]))
    gate1 = silu(qz1[:, head:])
    heads = wlog.shape[1] // 2
    lanes = lax.broadcasted_iota(jnp.int32, (1, 2 * heads), 1)
    is_beta = lanes == tp
    is_decay = lanes == tp + heads
    speed_lanes = lax.broadcasted_iota(jnp.int32, (1, heads), 1)
    speed = jnp.sum(
        jnp.where(speed_lanes == tp, speeds[...], 0.0), axis=1, keepdims=True
    )

    def pick(logits, which):
        return jnp.sum(jnp.where(which, logits, 0.0), axis=1, keepdims=True)

    b1 = sigmoid(pick(l1, is_beta))
    a1 = jnp.exp(-speed * softplus(pick(l1, is_decay)))
    kq = jnp.sum(k1 * q1, axis=-1, keepdims=True)
    query = a1 * (q1 - b1 * k1 * kq)
    own_write = b1 * v1 * kq

    loads[5].wait()

    def project(source, p, fresh=False):
        xs = buf[source, p]
        at_row = pl.ds(pl.multiple_of(source * feats, feats), feats)
        kv = mm(xs, wkv[at_row, :])
        lg = mm(xs, wlog[at_row, :])
        if fresh:
            acc[p] = kv
            lacc[p] = lg
        else:
            acc[p] += kv
            lacc[p] += lg

    for p in range(prompts):
        project(tp, p, True)
        if cube:
            arrived(near, p)
            go(gather_copy(near, p, far, 3))
            go(gather_copy(near, p, partner, 4))
            arrived(far, p)
            go(gather_copy(far, p, partner, 5))
            arrived(partner, p)
            project(partner, p)
            project(near, p)
            project(far, p)
            arrived(near2, p)
            project(near2, p)
            arrived(far2, p)
            project(far2, p)
            arrived(across, p)
            go(gather_copy(across, p, partner, 6))
            project(across, p)
            arrived(across2, p)
            project(across2, p)
        else:

            def one(d, carry):
                source = lax.rem(tp + d, n_tp)
                arrived(source, p)
                project(source, p)
                return carry

            lax.fori_loop(1, n_tp, one, 0)

        kv = acc[p]
        keys = unit(silu(kv[:, :head])).astype(BF)
        values = silu(kv[:, head:]).astype(BF)
        scores = lacc[p].astype(BF).astype(F32)
        beta = sigmoid(pick(scores, is_beta))
        fade = -speed * softplus(pick(scores, is_decay))
        cuts = [slice(b * block, (b + 1) * block) for b in range(length // block)]
        maps[p] = local_maps(
            [keys[c] for c in cuts],
            [values[c] for c in cuts],
            [beta[c] for c in cuts],
            [fade[c] for c in cuts],
            [extra[p : p + 1, c] for c in cuts],
        )

    hi_ = lax.broadcasted_iota(jnp.int32, (head, head), 0)
    hj_ = lax.broadcasted_iota(jnp.int32, (head, head), 1)
    heye = hi_ == hj_
    last_sp = n_sp - 1
    meet = max(n_sp // 2 - 1, 0)

    def chain_copy(p):
        return pltpu.make_async_remote_copy(
            src_ref=state_out.at[p],
            dst_ref=prev.at[p],
            send_sem=chain_send.at[p],
            recv_sem=chain_recv.at[p],
            device_id=(lax.rem(sp + 1, n_sp), tp),
            device_id_type=MESH,
        )

    def back_copy():
        return pltpu.make_async_remote_copy(
            src_ref=msg_out,
            dst_ref=msg_in,
            send_sem=back_send.at[0],
            recv_sem=back_recv.at[0],
            device_id=(lax.rem(sp + n_sp - 1, n_sp), tp),
            device_id_type=MESH,
        )

    def forward_first():
        for p in range(prompts):
            state_out[p] = maps[p][:, head:].astype(BF)
            if n_sp > 1:
                chain_copy(p).start()

    def forward_later(send):
        for p in range(prompts):
            chain_copy(p).wait_recv()
            both = maps[p]
            state = mm_split_left(both[:, :head], prev[p]) + both[:, head:]
            maps[p, :, head:] = state
            state_out[p] = state.astype(BF)
            if send:
                chain_copy(p).start()

    def back_step(message):
        for p in range(prompts):
            line = message[p : p + 1, :]
            col = to_col(line, heye)
            out = jnp.sum(col * maps[p], axis=0, keepdims=True)
            msg_out[p : p + 1, :] = out[:, :head]
            msg_out[prompts + p : prompts + p + 1, :] = (
                message[prompts + p : prompts + p + 1, :] + out[:, head:]
            )

    pl.when(sp == 0)(forward_first)
    if n_sp > 1:

        @pl.when(sp == last_sp)
        def _():
            back_step(jnp.concatenate([query, jnp.zeros_like(query)], axis=0))
            back_copy().start()

        if last_sp - meet > 1:

            @pl.when((sp > meet) & (sp < last_sp))
            def _():
                back_copy().wait_recv()
                back_step(msg_in[...])
                back_copy().start()

        if n_sp > 2:

            @pl.when((sp > 0) & (sp < last_sp))
            def _():
                forward_later(True)

    def read_copy(d, mine):
        return pltpu.make_async_remote_copy(
            src_ref=read_out,
            dst_ref=read_in,
            send_sem=read_send.at[d],
            recv_sem=read_recv.at[0],
            device_id=(lax.rem(sp + d, n_sp), tp),
            device_id_type=MESH,
        )

    @pl.when(sp == meet)
    def _():
        if n_sp > 1:
            back_copy().wait_recv()
            message = msg_in[...]
        else:
            message = jnp.concatenate([query, jnp.zeros_like(query)], axis=0)
        for p in range(prompts):
            col = to_col(message[p : p + 1, :], heye)
            out = jnp.sum(col * maps[p, :, head:], axis=0, keepdims=True)
            read = message[prompts + p : prompts + p + 1, :] + out
            read_out[p : p + 1, :] = read + own_write[p : p + 1, :]
        for d in range(1, n_sp):
            read_copy(d, True).start()
        read_in[...] = read_out[...]

    if n_sp > 1:

        @pl.when(sp != meet)
        def _():
            read_copy(0, False).wait_recv()

    read = read_in[...]
    normed = (
        read
        * lax.rsqrt(jnp.mean(read * read, axis=-1, keepdims=True) + EPS)
        * gain[...]
        * gate1
    ).astype(BF)
    loads[4].wait()
    shares = mm(normed, wexit[...])
    width = step_out.shape[1]
    for t in range(n_tp):
        part[t] = shares[:, t * width : (t + 1) * width]

    def part_copy(d):
        target = lax.rem(tp + d, n_tp)
        return pltpu.make_async_remote_copy(
            src_ref=part.at[target],
            dst_ref=parts.at[tp],
            send_sem=part_send.at[d],
            recv_sem=part_recv.at[tp],
            device_id=(sp, target),
            device_id_type=MESH,
        )

    def part_arrived(source):
        return pltpu.make_async_remote_copy(
            src_ref=part.at[0],
            dst_ref=parts.at[source],
            send_sem=part_send.at[0],
            recv_sem=part_recv.at[source],
            device_id=(sp, tp),
            device_id_type=MESH,
        )

    for d in range(1, n_tp):
        part_copy(d).start()
    parts[tp] = part[tp]

    if n_sp > 1:

        @pl.when(sp == last_sp)
        def _():
            forward_later(False)

    for d in range(1, n_tp):
        part_arrived(lax.rem(tp + d, n_tp)).wait_recv()
    total = parts[0]
    for t in range(1, n_tp):
        total = total + parts[t]
    step_out[...] = total.astype(BF)

    for copy in sends:
        copy.wait_send()
    for d in range(1, n_tp):
        part_copy(d).wait_send()
    if n_sp > 1:

        @pl.when(sp < last_sp)
        def _():
            for p in range(prompts):
                chain_copy(p).wait_send()

        @pl.when(sp > meet)
        def _():
            back_copy().wait_send()

        @pl.when(sp == meet)
        def _():
            for d in range(1, n_sp):
                read_copy(d, True).wait_send()


def body(
    n_sp,
    n_tp,
    context,
    first,
    wk,
    wv,
    wq,
    wz,
    w_write,
    w_fade,
    speeds,
    extra,
    gain,
    w_exit,
):
    head = gain.shape[0]
    prompts, length, feats = context.shape
    width = wk.shape[0]
    heads = w_write.shape[1]
    assert wk.shape[1] == head and heads == n_tp
    block = min(head, length)
    wlog = jnp.concatenate([w_write, w_fade], axis=1)
    vmem = pl.BlockSpec(memory_space=pltpu.VMEM)
    anym = pl.BlockSpec(memory_space=pl.ANY)
    dma = pltpu.SemaphoreType.DMA
    out_cols = w_exit.shape[1] // n_tp
    state, step = pl.pallas_call(
        functools.partial(kernel, n_sp, n_tp, block),
        name="delta",
        out_shape=(
            jax.ShapeDtypeStruct((prompts, head, head), BF),
            jax.ShapeDtypeStruct((prompts, out_cols), BF),
        ),
        in_specs=[anym, vmem, anym, anym, anym, anym, vmem, vmem, vmem, vmem, anym],
        out_specs=(vmem, vmem),
        scratch_shapes=[
            pltpu.VMEM((n_tp, prompts, length, feats), BF),
            pltpu.VMEM((width, 2 * head), BF),
            pltpu.VMEM((width, 2 * head), BF),
            pltpu.VMEM(w_exit.shape, BF),
            pltpu.VMEM((prompts, length, 2 * head), F32),
            pltpu.VMEM((prompts, length, 2 * heads), F32),
            pltpu.VMEM((prompts, head, 2 * head), F32),
            pltpu.VMEM((prompts, head, head), BF),
            pltpu.VMEM((2 * prompts, head), F32),
            pltpu.VMEM((2 * prompts, head), F32),
            pltpu.VMEM((prompts, head), F32),
            pltpu.VMEM((prompts, head), F32),
            pltpu.VMEM((n_tp, prompts, out_cols), F32),
            pltpu.VMEM((n_tp, prompts, out_cols), F32),
            dma((6,)),
            dma((max(n_tp, 7), prompts)),
            dma((n_tp, prompts)),
            dma((prompts,)),
            dma((prompts,)),
            dma((1,)),
            dma((1,)),
            dma((n_sp,)),
            dma((1,)),
            dma((n_tp,)),
            dma((n_tp,)),
        ],
        compiler_params=pltpu.CompilerParams(
            collective_id=0, has_side_effects=True, vmem_limit_bytes=60 * 2**20
        ),
    )(
        context,
        first,
        wk,
        wv,
        wq,
        wz,
        wlog,
        speeds.reshape(1, heads),
        extra.reshape(prompts, length),
        gain.reshape(1, head),
        w_exit,
    )
    return state[:, None, None], step


def solution(mesh):
    placed = (
        P(None, "sp", "tp"),
        P(),
        P(None, "tp"),
        P(None, "tp"),
        P(None, "tp"),
        P(None, "tp"),
        P(),
        P(),
        P(),
        P(None, "sp", "tp"),
        P(),
        P("tp", None),
    )
    return jax.shard_map(
        functools.partial(body, mesh.shape["sp"], mesh.shape["tp"]),
        mesh=mesh,
        in_specs=placed,
        out_specs=(P(None, "sp", "tp", None, None), P(None, "tp")),
        check_vma=False,
    )
```

```python
import functools

import jax
import jax.numpy as jnp
from jax import lax
from jax.experimental import pallas as pl
from jax.experimental.pallas import tpu as pltpu
from jax.sharding import PartitionSpec as P

EPS = 1e-06
BF = jnp.bfloat16
F32 = jnp.float32
MESH = pl.DeviceIdType.MESH


def mm(a, b, dims=((1,), (0,))):
    return lax.dot_general(a, b, (dims, ((), ())), preferred_element_type=F32)


def split(a):
    hi = a.astype(BF)
    return hi, (a - hi.astype(F32)).astype(BF)


def mm_split_left(a, b, dims=((1,), (0,))):
    hi, lo = split(a)
    return mm(hi, b, dims) + mm(lo, b, dims)


def mm_split_right(a, b):
    hi, lo = split(b)
    return mm(a, hi) + mm(a, lo)


def mm3(a, b):
    ah, al = split(a)
    bh, bl = split(b)
    return mm(ah, bh) + (mm(ah, bl) + mm(al, bh))


def silu(v):
    return v / (1.0 + jnp.exp(-v))


def sigmoid(v):
    return 1.0 / (1.0 + jnp.exp(-v))


def softplus(v):
    return jnp.maximum(v, 0.0) + jnp.log1p(jnp.exp(-jnp.abs(v)))


def unit(v):
    return v * lax.rsqrt(jnp.sum(v * v, axis=-1, keepdims=True) + EPS)


def to_col(row, eye):
    return jnp.sum(jnp.where(eye, row, 0.0), axis=1, keepdims=True)


def to_row(col, eye):
    return jnp.sum(jnp.where(eye, col, 0.0), axis=0, keepdims=True)


def local_maps(keys, values, beta, log_decay, extra):
    n = keys[0].shape[0]
    i = lax.broadcasted_iota(jnp.int32, (n, n), 0)
    j = lax.broadcasted_iota(jnp.int32, (n, n), 1)
    eye = i == j
    blocks = range(len(keys))
    rows, cols, systems, solved = [], [], [], []
    for b in blocks:
        fade = log_decay[b] + to_col(extra[b], eye)
        c_row = jnp.sum(jnp.where(i <= j, fade, 0.0), axis=0, keepdims=True)
        c_col = to_col(c_row, eye)
        gram = mm(keys[b], keys[b], ((1,), (1,)))
        within = jnp.exp(jnp.where(i > j, c_col - c_row, 0.0))
        systems.append(jnp.where(i > j, beta[b] * gram * within, 0.0))
        rows.append(c_row)
        cols.append(c_col)
    for b in blocks:
        solved.append(
            jnp.where(eye, 1.0, 0.0) - jnp.where((i // 2) == (j // 2), systems[b], 0.0)
        )
    size = 2
    while size < n:
        mask = ((i // (2 * size)) == (j // (2 * size))) & ((i // size) != (j // size))
        half = [mm3(jnp.where(mask, systems[b], 0.0), solved[b]) for b in blocks]
        solved = [solved[b] - mm3(solved[b], half[b]) for b in blocks]
        size *= 2
    total = None
    for b in blocks:
        beta_row = to_row(beta[b], eye)
        scaled = solved[b] * beta_row
        pseudo = mm_split_left(scaled, values[b])
        decayed = mm_split_left(scaled * jnp.exp(rows[b]), keys[b])
        last = cols[b][n - 1 : n, :]
        trail = jnp.exp(last - cols[b])
        both = jnp.concatenate([-decayed, pseudo], axis=1) * trail
        hi, lo = split(both)
        turned = ((0,), (0,))
        both = mm(keys[b], hi, turned) + mm(keys[b], lo, turned)
        width = keys[b].shape[1]
        wi = lax.broadcasted_iota(jnp.int32, (width, both.shape[1]), 0)
        wj = lax.broadcasted_iota(jnp.int32, (width, both.shape[1]), 1)
        both = both + jnp.where(wi == wj, jnp.exp(last), 0.0)
        if total is None:
            total = both
        else:
            width_off = jnp.where(wj >= width, both, 0.0)
            total = mm3(both[:, :width], total) + width_off
    return total


def kernel(
    n_sp,
    n_tp,
    block,
    ctx,
    first,
    wk_hbm,
    wv_hbm,
    wq_hbm,
    wz_hbm,
    w_write,
    w_fade,
    speeds,
    extra,
    gain,
    exit_hbm,
    state_out,
    step_out,
    buf,
    wkv,
    wqz,
    wexit,
    acc,
    bacc,
    facc,
    maps,
    sent,
    prev,
    msg_out,
    msg_in,
    read_out,
    read_in,
    part,
    parts,
    local_sem,
    send_sem,
    recv_sem,
    chain_send,
    chain_recv,
    back_send,
    back_recv,
    read_send,
    read_recv,
    part_send,
    part_recv,
):
    prompts, length, feats = ctx.shape
    head = wk_hbm.shape[1]
    sp = lax.axis_index("sp")
    tp = lax.axis_index("tp")
    pairs = [(wk_hbm, wkv, 0), (wv_hbm, wkv, 1), (wq_hbm, wqz, 0), (wz_hbm, wqz, 1)]
    loads = [
        pltpu.make_async_copy(src, dst.at[:, pl.ds(at * head, head)], local_sem.at[k])
        for k, (src, dst, at) in enumerate(pairs)
    ]
    loads.append(pltpu.make_async_copy(exit_hbm, wexit, local_sem.at[4]))
    loads.append(pltpu.make_async_copy(ctx, buf.at[tp], local_sem.at[5]))
    loads[5].start()
    for copy in loads[:5]:
        copy.start()

    barrier = pltpu.get_barrier_semaphore()
    for d in range(1, n_tp):
        pl.semaphore_signal(
            barrier, inc=1, device_id=(sp, lax.rem(tp + d, n_tp)), device_id_type=MESH
        )
    for d in range(1, n_sp):
        pl.semaphore_signal(
            barrier, inc=1, device_id=(lax.rem(sp + d, n_sp), tp), device_id_type=MESH
        )
    loads[5].wait()
    pl.semaphore_wait(barrier, n_tp + n_sp - 2)

    def gather_copy(source, p, target, k):
        return pltpu.make_async_remote_copy(
            src_ref=buf.at[source, p],
            dst_ref=buf.at[source, p],
            send_sem=send_sem.at[k, p],
            recv_sem=recv_sem.at[source, p],
            device_id=(sp, target),
            device_id_type=MESH,
        )

    sends = []

    def go(copy):
        copy.start()
        sends.append(copy)

    def arrived(source, p):
        gather_copy(source, p, tp, 0).wait_recv()

    cube = n_tp == 8
    if cube:
        y, x, core = tp // 4, (tp // 2) % 2, tp % 2

        def at(yy, xx, cc):
            return yy * 4 + xx * 2 + cc

        def turn(yy, xx, cc, first_axis):
            on_x = (1 - cc) if first_axis else cc
            on_y = cc if first_axis else (1 - cc)
            return yy + on_y * (1 - 2 * yy), xx + on_x * (1 - 2 * xx)

        near = at(*turn(y, x, core, True), core)
        far = at(*turn(y, x, core, False), core)
        across = at(1 - y, 1 - x, core)
        partner = at(y, x, 1 - core)
        near2 = at(*turn(y, x, 1 - core, True), 1 - core)
        far2 = at(*turn(y, x, 1 - core, False), 1 - core)
        across2 = at(1 - y, 1 - x, 1 - core)
        for p in range(prompts):
            go(gather_copy(tp, p, near, 0))
            if p == 0:
                go(gather_copy(tp, p, far, 1))
            go(gather_copy(tp, p, partner, 2))
    else:
        for p in range(prompts):
            for d in range(1, n_tp):
                go(gather_copy(tp, p, lax.rem(tp + d, n_tp), d))

    for copy in loads[:4]:
        copy.wait()
    x1 = first[...]
    kv1 = mm(x1, wkv[...])
    qz1 = mm(x1, wqz[...])
    turned = ((1,), (1,))
    lb1 = mm(x1, w_write[...], turned)
    lf1 = mm(x1, w_fade[...], turned)
    k1 = unit(silu(kv1[:, :head]))
    v1 = silu(kv1[:, head:])
    q1 = unit(silu(qz1[:, :head]))
    gate1 = silu(qz1[:, head:])
    heads = w_write.shape[0]
    mine = lax.broadcasted_iota(jnp.int32, (1, heads), 1) == tp

    def pick(logits):
        return jnp.sum(jnp.where(mine, logits, 0.0), axis=1, keepdims=True)

    speed = pick(speeds[...])
    b1 = sigmoid(pick(lb1))
    a1 = jnp.exp(-speed * softplus(pick(lf1)))
    kq = jnp.sum(k1 * q1, axis=-1, keepdims=True)
    query = a1 * (q1 - b1 * k1 * kq)
    own_write = b1 * v1 * kq

    def project(source, p, fresh=False):
        xs = buf[source, p]
        at_row = pl.ds(pl.multiple_of(source * feats, feats), feats)
        kv = mm(xs, wkv[at_row, :])
        lb = mm(xs, w_write[:, at_row], turned)
        lf = mm(xs, w_fade[:, at_row], turned)
        if fresh:
            acc[p] = kv
            bacc[p] = lb
            facc[p] = lf
        else:
            acc[p] += kv
            bacc[p] += lb
            facc[p] += lf

    hi_ = lax.broadcasted_iota(jnp.int32, (head, head), 0)
    hj_ = lax.broadcasted_iota(jnp.int32, (head, head), 1)
    heye = hi_ == hj_
    last_sp = n_sp - 1
    meet = max(n_sp // 2 - 1, 0)

    def chain_copy(p):
        return pltpu.make_async_remote_copy(
            src_ref=sent.at[p],
            dst_ref=prev.at[p],
            send_sem=chain_send.at[p],
            recv_sem=chain_recv.at[p],
            device_id=(lax.rem(sp + 1, n_sp), tp),
            device_id_type=MESH,
        )

    def back_copy():
        return pltpu.make_async_remote_copy(
            src_ref=msg_out,
            dst_ref=msg_in,
            send_sem=back_send.at[0],
            recv_sem=back_recv.at[0],
            device_id=(lax.rem(sp + n_sp - 1, n_sp), tp),
            device_id_type=MESH,
        )

    def forward_first(p):
        state_out[p] = maps[p, :, head:]
        sent[p] = maps[p, :, head:].astype(BF)
        if n_sp > 1:
            chain_copy(p).start()

    def forward_later(send):
        for p in range(prompts):
            chain_copy(p).wait_recv()
            both = maps[p]
            state = mm_split_left(both[:, :head], prev[p]) + both[:, head:]
            maps[p, :, head:] = state
            state_out[p] = state
            if send:
                sent[p] = state.astype(BF)
                chain_copy(p).start()

    def back_step(message):
        for p in range(prompts):
            line = message[p : p + 1, :]
            col = to_col(line, heye)
            out = jnp.sum(col * maps[p], axis=0, keepdims=True)
            msg_out[p : p + 1, :] = out[:, :head]
            msg_out[prompts + p : prompts + p + 1, :] = (
                message[prompts + p : prompts + p + 1, :] + out[:, head:]
            )

    for p in range(prompts):
        project(tp, p, True)
        if cube:
            arrived(near, p)
            go(gather_copy(near, p, far, 3))
            if p + 1 < prompts:
                go(gather_copy(tp, p + 1, far, 1))
            go(gather_copy(near, p, partner, 4))
            arrived(far, p)
            go(gather_copy(far, p, partner, 5))
            arrived(partner, p)
            project(partner, p)
            project(near, p)
            project(far, p)
            arrived(near2, p)
            project(near2, p)
            arrived(far2, p)
            project(far2, p)
            arrived(across, p)
            go(gather_copy(across, p, partner, 6))
            project(across, p)
            arrived(across2, p)
            project(across2, p)
        else:

            def one(d, carry):
                source = lax.rem(tp + d, n_tp)
                arrived(source, p)
                project(source, p)
                return carry

            lax.fori_loop(1, n_tp, one, 0)

        kv = acc[p]
        keys = unit(silu(kv[:, :head])).astype(BF)
        values = silu(kv[:, head:]).astype(BF)
        beta = sigmoid(pick(bacc[p].astype(BF).astype(F32)))
        fade = -speed * softplus(pick(facc[p].astype(BF).astype(F32)))
        cuts = [slice(b * block, (b + 1) * block) for b in range(length // block)]
        maps[p] = local_maps(
            [keys[c] for c in cuts],
            [values[c] for c in cuts],
            [beta[c] for c in cuts],
            [fade[c] for c in cuts],
            [extra[p, :, c] for c in cuts],
        )
        pl.when(sp == 0)(functools.partial(forward_first, p))

    if n_sp > 1:

        @pl.when(sp == last_sp)
        def _():
            back_step(jnp.concatenate([query, jnp.zeros_like(query)], axis=0))
            back_copy().start()

        if last_sp - meet > 1:

            @pl.when((sp > meet) & (sp < last_sp))
            def _():
                back_copy().wait_recv()
                back_step(msg_in[...])
                back_copy().start()

        if n_sp > 2:

            @pl.when((sp > 0) & (sp < last_sp))
            def _():
                forward_later(True)

    def read_copy(d, mine):
        return pltpu.make_async_remote_copy(
            src_ref=read_out,
            dst_ref=read_in,
            send_sem=read_send.at[d],
            recv_sem=read_recv.at[0],
            device_id=(lax.rem(sp + d, n_sp), tp),
            device_id_type=MESH,
        )

    @pl.when(sp == meet)
    def _():
        if n_sp > 1:
            back_copy().wait_recv()
            message = msg_in[...]
        else:
            message = jnp.concatenate([query, jnp.zeros_like(query)], axis=0)
        for p in range(prompts):
            col = to_col(message[p : p + 1, :], heye)
            out = jnp.sum(col * maps[p, :, head:], axis=0, keepdims=True)
            read = message[prompts + p : prompts + p + 1, :] + out
            read_out[p : p + 1, :] = read + own_write[p : p + 1, :]
        for d in range(1, n_sp):
            read_copy(d, True).start()
        read_in[...] = read_out[...]

    if n_sp > 1:

        @pl.when(sp != meet)
        def _():
            read_copy(0, False).wait_recv()

    read = read_in[...]
    normed = (
        read
        * lax.rsqrt(jnp.mean(read * read, axis=-1, keepdims=True) + EPS)
        * gain[...]
        * gate1
    ).astype(BF)
    loads[4].wait()
    shares = mm(normed, wexit[...])
    width = step_out.shape[1]
    for t in range(n_tp):
        part[t] = shares[:, t * width : (t + 1) * width]

    def part_copy(d):
        target = lax.rem(tp + d, n_tp)
        return pltpu.make_async_remote_copy(
            src_ref=part.at[target],
            dst_ref=parts.at[tp],
            send_sem=part_send.at[d],
            recv_sem=part_recv.at[tp],
            device_id=(sp, target),
            device_id_type=MESH,
        )

    def part_arrived(source):
        return pltpu.make_async_remote_copy(
            src_ref=part.at[0],
            dst_ref=parts.at[source],
            send_sem=part_send.at[0],
            recv_sem=part_recv.at[source],
            device_id=(sp, tp),
            device_id_type=MESH,
        )

    for d in range(1, n_tp):
        part_copy(d).start()
    parts[tp] = part[tp]

    if n_sp > 1:

        @pl.when(sp == last_sp)
        def _():
            forward_later(False)

    for d in range(1, n_tp):
        part_arrived(lax.rem(tp + d, n_tp)).wait_recv()
    total = parts[0]
    for t in range(1, n_tp):
        total = total + parts[t]
    step_out[...] = total

    for copy in sends:
        copy.wait_send()
    for d in range(1, n_tp):
        part_copy(d).wait_send()
    if n_sp > 1:

        @pl.when(sp < last_sp)
        def _():
            for p in range(prompts):
                chain_copy(p).wait_send()

        @pl.when(sp > meet)
        def _():
            back_copy().wait_send()

        @pl.when(sp == meet)
        def _():
            for d in range(1, n_sp):
                read_copy(d, True).wait_send()


def body(
    n_sp,
    n_tp,
    context,
    first,
    wk,
    wv,
    wq,
    wz,
    w_write,
    w_fade,
    speeds,
    extra,
    gain,
    w_exit,
):
    head = gain.shape[0]
    prompts, length, feats = context.shape
    width = wk.shape[0]
    heads = w_write.shape[1]
    assert wk.shape[1] == head and heads == n_tp
    block = min(head, length)
    vmem = pl.BlockSpec(memory_space=pltpu.VMEM)
    anym = pl.BlockSpec(memory_space=pl.ANY)
    dma = pltpu.SemaphoreType.DMA
    out_cols = w_exit.shape[1] // n_tp
    state, step = pl.pallas_call(
        functools.partial(kernel, n_sp, n_tp, block),
        name="delta",
        out_shape=(
            jax.ShapeDtypeStruct((prompts, head, head), F32),
            jax.ShapeDtypeStruct((prompts, out_cols), F32),
        ),
        in_specs=[anym, vmem] + [anym] * 4 + [vmem] * 5 + [anym],
        out_specs=(vmem, vmem),
        scratch_shapes=[
            pltpu.VMEM((n_tp, prompts, length, feats), BF),
            pltpu.VMEM((width, 2 * head), BF),
            pltpu.VMEM((width, 2 * head), BF),
            pltpu.VMEM(w_exit.shape, BF),
            pltpu.VMEM((prompts, length, 2 * head), F32),
            pltpu.VMEM((prompts, length, heads), F32),
            pltpu.VMEM((prompts, length, heads), F32),
            pltpu.VMEM((prompts, head, 2 * head), F32),
            pltpu.VMEM((prompts, head, head), BF),
            pltpu.VMEM((prompts, head, head), BF),
            pltpu.VMEM((2 * prompts, head), F32),
            pltpu.VMEM((2 * prompts, head), F32),
            pltpu.VMEM((prompts, head), F32),
            pltpu.VMEM((prompts, head), F32),
            pltpu.VMEM((n_tp, prompts, out_cols), F32),
            pltpu.VMEM((n_tp, prompts, out_cols), F32),
            dma((6,)),
            dma((max(n_tp, 7), prompts)),
            dma((n_tp, prompts)),
            dma((prompts,)),
            dma((prompts,)),
            dma((1,)),
            dma((1,)),
            dma((n_sp,)),
            dma((1,)),
            dma((n_tp,)),
            dma((n_tp,)),
        ],
        compiler_params=pltpu.CompilerParams(
            collective_id=0, has_side_effects=True, vmem_limit_bytes=64 * 2**20 - 420 * 2**10
        ),
    )(
        context,
        first,
        wk,
        wv,
        wq,
        wz,
        w_write.T,
        w_fade.T,
        speeds.reshape(1, heads),
        extra.reshape(prompts, 1, length),
        gain.reshape(1, head),
        w_exit,
    )
    return state[:, None, None].astype(BF), step.astype(BF)


def solution(mesh):
    placed = (
        P(None, "sp", "tp"),
        P(),
        P(None, "tp"),
        P(None, "tp"),
        P(None, "tp"),
        P(None, "tp"),
        P(),
        P(),
        P(),
        P(None, "sp", "tp"),
        P(),
        P("tp", None),
    )
    return jax.shard_map(
        functools.partial(body, mesh.shape["sp"], mesh.shape["tp"]),
        mesh=mesh,
        in_specs=placed,
        out_specs=(P(None, "sp", "tp", None, None), P(None, "tp")),
        check_vma=False,
    )
```

```python
import functools

import jax
import jax.numpy as jnp
from jax import lax
from jax.experimental import pallas as pl
from jax.experimental.pallas import tpu as pltpu
from jax.sharding import PartitionSpec as P

EPS = 1e-06
BF = jnp.bfloat16
F32 = jnp.float32
MESH = pl.DeviceIdType.MESH


def mm(a, b, dims=((1,), (0,))):
    return lax.dot_general(a, b, (dims, ((), ())), preferred_element_type=F32)


def split(a):
    hi = a.astype(BF)
    return hi, (a - hi.astype(F32)).astype(BF)


def mm_split_left(a, b, dims=((1,), (0,))):
    hi, lo = split(a)
    return mm(hi, b, dims) + mm(lo, b, dims)


def mm_split_right(a, b):
    hi, lo = split(b)
    return mm(a, hi) + mm(a, lo)


def mm3(a, b):
    ah, al = split(a)
    bh, bl = split(b)
    return mm(ah, bh) + (mm(ah, bl) + mm(al, bh))


def silu(v):
    return v / (1.0 + jnp.exp(-v))


def sigmoid(v):
    return 1.0 / (1.0 + jnp.exp(-v))


def softplus(v):
    return jnp.maximum(v, 0.0) + jnp.log1p(jnp.exp(-jnp.abs(v)))


def unit(v):
    return v * lax.rsqrt(jnp.sum(v * v, axis=-1, keepdims=True) + EPS)


def to_col(row, eye):
    return jnp.sum(jnp.where(eye, row, 0.0), axis=1, keepdims=True)


def to_row(col, eye):
    return jnp.sum(jnp.where(eye, col, 0.0), axis=0, keepdims=True)


def local_maps(keys, values, beta, log_decay, extra):
    n = keys[0].shape[0]
    i = lax.broadcasted_iota(jnp.int32, (n, n), 0)
    j = lax.broadcasted_iota(jnp.int32, (n, n), 1)
    eye = i == j
    blocks = range(len(keys))
    rows, cols, systems, solved = [], [], [], []
    for b in blocks:
        fade = log_decay[b] + to_col(extra[b], eye)
        c_row = jnp.sum(jnp.where(i <= j, fade, 0.0), axis=0, keepdims=True)
        c_col = to_col(c_row, eye)
        gram = mm(keys[b], keys[b], ((1,), (1,)))
        within = jnp.exp(jnp.where(i > j, c_col - c_row, 0.0))
        systems.append(jnp.where(i > j, beta[b] * gram * within, 0.0))
        rows.append(c_row)
        cols.append(c_col)
    for b in blocks:
        solved.append(
            jnp.where(eye, 1.0, 0.0) - jnp.where((i // 2) == (j // 2), systems[b], 0.0)
        )
    size = 2
    while size < n:
        mask = ((i // (2 * size)) == (j // (2 * size))) & ((i // size) != (j // size))
        half = [mm3(jnp.where(mask, systems[b], 0.0), solved[b]) for b in blocks]
        solved = [solved[b] - mm3(solved[b], half[b]) for b in blocks]
        size *= 2
    total = None
    for b in blocks:
        beta_row = to_row(beta[b], eye)
        scaled = solved[b] * beta_row
        pseudo = mm_split_left(scaled, values[b])
        decayed = mm_split_left(scaled * jnp.exp(rows[b]), keys[b])
        last = cols[b][n - 1 : n, :]
        trail = jnp.exp(last - cols[b])
        both = jnp.concatenate([-decayed, pseudo], axis=1) * trail
        hi, lo = split(both)
        turned = ((0,), (0,))
        both = mm(keys[b], hi, turned) + mm(keys[b], lo, turned)
        width = keys[b].shape[1]
        wi = lax.broadcasted_iota(jnp.int32, (width, both.shape[1]), 0)
        wj = lax.broadcasted_iota(jnp.int32, (width, both.shape[1]), 1)
        both = both + jnp.where(wi == wj, jnp.exp(last), 0.0)
        if total is None:
            total = both
        else:
            width_off = jnp.where(wj >= width, both, 0.0)
            total = mm3(both[:, :width], total) + width_off
    return total


def kernel(
    n_sp,
    n_tp,
    block,
    ctx,
    first_hbm,
    wk_hbm,
    wv_hbm,
    wq_hbm,
    wz_hbm,
    write_hbm,
    fade_hbm,
    speeds_hbm,
    extra_hbm,
    gain_hbm,
    exit_hbm,
    state_out,
    step_out,
    first,
    w_write,
    w_fade,
    speeds,
    extra,
    gain,
    buf,
    wkv,
    wqz,
    wexit,
    acc,
    bacc,
    facc,
    maps,
    sent,
    prev,
    msg_out,
    msg_in,
    read_out,
    read_in,
    part,
    parts,
    local_sem,
    send_sem,
    recv_sem,
    chain_send,
    chain_recv,
    back_send,
    back_recv,
    read_send,
    read_recv,
    part_send,
    part_recv,
):
    prompts, length, feats = ctx.shape
    head = wk_hbm.shape[1]
    sp = lax.axis_index("sp")
    tp = lax.axis_index("tp")
    pairs = [(wk_hbm, wkv, 0), (wv_hbm, wkv, 1), (wq_hbm, wqz, 0), (wz_hbm, wqz, 1)]
    loads = [
        pltpu.make_async_copy(src, dst.at[:, pl.ds(at * head, head)], local_sem.at[k])
        for k, (src, dst, at) in enumerate(pairs)
    ]
    loads.append(pltpu.make_async_copy(exit_hbm, wexit, local_sem.at[4]))
    loads.append(pltpu.make_async_copy(ctx, buf.at[tp], local_sem.at[5]))
    loads[5].start()
    few = [
        (first_hbm, first),
        (write_hbm, w_write),
        (fade_hbm, w_fade),
        (speeds_hbm, speeds),
        (extra_hbm, extra),
        (gain_hbm, gain),
    ]
    small = [
        pltpu.make_async_copy(src, dst, local_sem.at[6 + k])
        for k, (src, dst) in enumerate(few)
    ]
    for copy in small:
        copy.start()
    for copy in loads[:5]:
        copy.start()

    barrier = pltpu.get_barrier_semaphore()
    for d in range(1, n_tp):
        pl.semaphore_signal(
            barrier, inc=1, device_id=(sp, lax.rem(tp + d, n_tp)), device_id_type=MESH
        )
    for d in range(1, n_sp):
        pl.semaphore_signal(
            barrier, inc=1, device_id=(lax.rem(sp + d, n_sp), tp), device_id_type=MESH
        )
    loads[5].wait()
    pl.semaphore_wait(barrier, n_tp + n_sp - 2)

    def gather_copy(source, p, target, k):
        return pltpu.make_async_remote_copy(
            src_ref=buf.at[source, p],
            dst_ref=buf.at[source, p],
            send_sem=send_sem.at[k, p],
            recv_sem=recv_sem.at[source, p],
            device_id=(sp, target),
            device_id_type=MESH,
        )

    sends = []

    def go(copy):
        copy.start()
        sends.append(copy)

    def arrived(source, p):
        gather_copy(source, p, tp, 0).wait_recv()

    cube = n_tp == 8
    if cube:
        y, x, core = tp // 4, (tp // 2) % 2, tp % 2

        def at(yy, xx, cc):
            return yy * 4 + xx * 2 + cc

        def turn(yy, xx, cc, first_axis):
            on_x = (1 - cc) if first_axis else cc
            on_y = cc if first_axis else (1 - cc)
            return yy + on_y * (1 - 2 * yy), xx + on_x * (1 - 2 * xx)

        near = at(*turn(y, x, core, True), core)
        far = at(*turn(y, x, core, False), core)
        across = at(1 - y, 1 - x, core)
        partner = at(y, x, 1 - core)
        near2 = at(*turn(y, x, 1 - core, True), 1 - core)
        far2 = at(*turn(y, x, 1 - core, False), 1 - core)
        across2 = at(1 - y, 1 - x, 1 - core)
        for p in range(prompts):
            go(gather_copy(tp, p, near, 0))
            if p == 0:
                go(gather_copy(tp, p, far, 1))
            go(gather_copy(tp, p, partner, 2))
    else:
        for p in range(prompts):
            for d in range(1, n_tp):
                go(gather_copy(tp, p, lax.rem(tp + d, n_tp), d))

    for copy in loads[:4] + small:
        copy.wait()
    x1 = first[...]
    kv1 = mm(x1, wkv[...])
    qz1 = mm(x1, wqz[...])
    turned = ((1,), (1,))
    lb1 = mm(x1, w_write[...], turned)
    lf1 = mm(x1, w_fade[...], turned)
    k1 = unit(silu(kv1[:, :head]))
    v1 = silu(kv1[:, head:])
    q1 = unit(silu(qz1[:, :head]))
    gate1 = silu(qz1[:, head:])
    heads = w_write.shape[0]
    mine = lax.broadcasted_iota(jnp.int32, (1, heads), 1) == tp

    def pick(logits):
        return jnp.sum(jnp.where(mine, logits, 0.0), axis=1, keepdims=True)

    speed = pick(speeds[...])
    b1 = sigmoid(pick(lb1))
    a1 = jnp.exp(-speed * softplus(pick(lf1)))
    kq = jnp.sum(k1 * q1, axis=-1, keepdims=True)
    query = a1 * (q1 - b1 * k1 * kq)
    own_write = b1 * v1 * kq

    def project(source, p, fresh=False):
        xs = buf[source, p]
        at_row = pl.ds(pl.multiple_of(source * feats, feats), feats)
        kv = mm(xs, wkv[at_row, :])
        lb = mm(xs, w_write[:, at_row], turned)
        lf = mm(xs, w_fade[:, at_row], turned)
        if fresh:
            acc[p] = kv
            bacc[p] = lb
            facc[p] = lf
        else:
            acc[p] += kv
            bacc[p] += lb
            facc[p] += lf

    hi_ = lax.broadcasted_iota(jnp.int32, (head, head), 0)
    hj_ = lax.broadcasted_iota(jnp.int32, (head, head), 1)
    heye = hi_ == hj_
    last_sp = n_sp - 1
    meet = max(n_sp // 2 - 1, 0)

    def chain_copy(p):
        return pltpu.make_async_remote_copy(
            src_ref=sent.at[p],
            dst_ref=prev.at[p],
            send_sem=chain_send.at[p],
            recv_sem=chain_recv.at[p],
            device_id=(lax.rem(sp + 1, n_sp), tp),
            device_id_type=MESH,
        )

    def back_copy():
        return pltpu.make_async_remote_copy(
            src_ref=msg_out,
            dst_ref=msg_in,
            send_sem=back_send.at[0],
            recv_sem=back_recv.at[0],
            device_id=(lax.rem(sp + n_sp - 1, n_sp), tp),
            device_id_type=MESH,
        )

    def forward_first(p):
        state_out[p] = maps[p, :, head:]
        sent[p] = maps[p, :, head:].astype(BF)
        if n_sp > 1:
            chain_copy(p).start()

    def forward_later(send):
        for p in range(prompts):
            chain_copy(p).wait_recv()
            both = maps[p]
            state = mm_split_left(both[:, :head], prev[p]) + both[:, head:]
            maps[p, :, head:] = state
            state_out[p] = state
            if send:
                sent[p] = state.astype(BF)
                chain_copy(p).start()

    def back_step(message):
        for p in range(prompts):
            line = message[p : p + 1, :]
            col = to_col(line, heye)
            out = jnp.sum(col * maps[p], axis=0, keepdims=True)
            msg_out[p : p + 1, :] = out[:, :head]
            msg_out[prompts + p : prompts + p + 1, :] = (
                message[prompts + p : prompts + p + 1, :] + out[:, head:]
            )

    def relay(p):
        arrived(near, p)
        go(gather_copy(near, p, far, 3))
        if p + 1 < prompts:
            go(gather_copy(tp, p + 1, far, 1))
        go(gather_copy(near, p, partner, 4))

    for p in range(prompts):
        project(tp, p, True)
        if cube:
            if p == 0:
                relay(p)
            arrived(far, p)
            go(gather_copy(far, p, partner, 5))
            arrived(partner, p)
            project(partner, p)
            project(near, p)
            project(far, p)
            arrived(near2, p)
            project(near2, p)
            arrived(far2, p)
            project(far2, p)
            arrived(across, p)
            go(gather_copy(across, p, partner, 6))
            project(across, p)
            arrived(across2, p)
            project(across2, p)
            if p + 1 < prompts:
                relay(p + 1)
        else:

            def one(d, carry):
                source = lax.rem(tp + d, n_tp)
                arrived(source, p)
                project(source, p)
                return carry

            lax.fori_loop(1, n_tp, one, 0)

        kv = acc[p]
        keys = unit(silu(kv[:, :head])).astype(BF)
        values = silu(kv[:, head:]).astype(BF)
        beta = sigmoid(pick(bacc[p].astype(BF).astype(F32)))
        fade = -speed * softplus(pick(facc[p].astype(BF).astype(F32)))
        cuts = [slice(b * block, (b + 1) * block) for b in range(length // block)]
        maps[p] = local_maps(
            [keys[c] for c in cuts],
            [values[c] for c in cuts],
            [beta[c] for c in cuts],
            [fade[c] for c in cuts],
            [extra[p, :, c] for c in cuts],
        )
        pl.when(sp == 0)(functools.partial(forward_first, p))

    if n_sp > 1:

        @pl.when(sp == last_sp)
        def _():
            back_step(jnp.concatenate([query, jnp.zeros_like(query)], axis=0))
            back_copy().start()

        if last_sp - meet > 1:

            @pl.when((sp > meet) & (sp < last_sp))
            def _():
                back_copy().wait_recv()
                back_step(msg_in[...])
                back_copy().start()

        if n_sp > 2:

            @pl.when((sp > 0) & (sp < last_sp))
            def _():
                forward_later(True)

    def read_copy(d, mine):
        return pltpu.make_async_remote_copy(
            src_ref=read_out,
            dst_ref=read_in,
            send_sem=read_send.at[d],
            recv_sem=read_recv.at[0],
            device_id=(lax.rem(sp + d, n_sp), tp),
            device_id_type=MESH,
        )

    @pl.when(sp == meet)
    def _():
        if n_sp > 1:
            back_copy().wait_recv()
            message = msg_in[...]
        else:
            message = jnp.concatenate([query, jnp.zeros_like(query)], axis=0)
        for p in range(prompts):
            col = to_col(message[p : p + 1, :], heye)
            out = jnp.sum(col * maps[p, :, head:], axis=0, keepdims=True)
            read = message[prompts + p : prompts + p + 1, :] + out
            read_out[p : p + 1, :] = read + own_write[p : p + 1, :]
        for d in range(1, n_sp):
            read_copy(d, True).start()
        read_in[...] = read_out[...]

    if n_sp > 1:

        @pl.when(sp != meet)
        def _():
            read_copy(0, False).wait_recv()

    read = read_in[...]
    normed = (
        read
        * lax.rsqrt(jnp.mean(read * read, axis=-1, keepdims=True) + EPS)
        * gain[...]
        * gate1
    ).astype(BF)
    loads[4].wait()
    shares = mm(normed, wexit[...])
    width = step_out.shape[1]
    for t in range(n_tp):
        part[t] = shares[:, t * width : (t + 1) * width]

    def part_copy(d):
        target = lax.rem(tp + d, n_tp)
        return pltpu.make_async_remote_copy(
            src_ref=part.at[target],
            dst_ref=parts.at[tp],
            send_sem=part_send.at[d],
            recv_sem=part_recv.at[tp],
            device_id=(sp, target),
            device_id_type=MESH,
        )

    def part_arrived(source):
        return pltpu.make_async_remote_copy(
            src_ref=part.at[0],
            dst_ref=parts.at[source],
            send_sem=part_send.at[0],
            recv_sem=part_recv.at[source],
            device_id=(sp, tp),
            device_id_type=MESH,
        )

    for d in range(1, n_tp):
        part_copy(d).start()
    parts[tp] = part[tp]

    if n_sp > 1:

        @pl.when(sp == last_sp)
        def _():
            forward_later(False)

    for d in range(1, n_tp):
        part_arrived(lax.rem(tp + d, n_tp)).wait_recv()
    total = parts[0]
    for t in range(1, n_tp):
        total = total + parts[t]
    step_out[...] = total

    for copy in sends:
        copy.wait_send()
    for d in range(1, n_tp):
        part_copy(d).wait_send()
    if n_sp > 1:

        @pl.when(sp < last_sp)
        def _():
            for p in range(prompts):
                chain_copy(p).wait_send()

        @pl.when(sp > meet)
        def _():
            back_copy().wait_send()

        @pl.when(sp == meet)
        def _():
            for d in range(1, n_sp):
                read_copy(d, True).wait_send()


def body(
    n_sp,
    n_tp,
    context,
    first,
    wk,
    wv,
    wq,
    wz,
    w_write,
    w_fade,
    speeds,
    extra,
    gain,
    w_exit,
):
    head = gain.shape[0]
    prompts, length, feats = context.shape
    width = wk.shape[0]
    heads = w_write.shape[1]
    assert wk.shape[1] == head and heads == n_tp
    block = min(head, length)
    vmem = pl.BlockSpec(memory_space=pltpu.VMEM)
    anym = pl.BlockSpec(memory_space=pltpu.HBM)
    dma = pltpu.SemaphoreType.DMA
    out_cols = w_exit.shape[1] // n_tp
    state, step = pl.pallas_call(
        functools.partial(kernel, n_sp, n_tp, block),
        name="delta",
        out_shape=(
            pltpu.VMEM((prompts, head, head), F32),
            pltpu.VMEM((prompts, out_cols), F32),
        ),
        in_specs=[anym] * 12,
        out_specs=(vmem, vmem),
        scratch_shapes=[
            pltpu.VMEM(first.shape, BF),
            pltpu.VMEM(w_write.shape[::-1], BF),
            pltpu.VMEM(w_fade.shape[::-1], BF),
            pltpu.VMEM((1, heads), F32),
            pltpu.VMEM((prompts, 1, length), F32),
            pltpu.VMEM((1, head), F32),
            pltpu.VMEM((n_tp, prompts, length, feats), BF),
            pltpu.VMEM((width, 2 * head), BF),
            pltpu.VMEM((width, 2 * head), BF),
            pltpu.VMEM(w_exit.shape, BF),
            pltpu.VMEM((prompts, length, 2 * head), F32),
            pltpu.VMEM((prompts, length, heads), F32),
            pltpu.VMEM((prompts, length, heads), F32),
            pltpu.VMEM((prompts, head, 2 * head), F32),
            pltpu.VMEM((prompts, head, head), BF),
            pltpu.VMEM((prompts, head, head), BF),
            pltpu.VMEM((2 * prompts, head), F32),
            pltpu.VMEM((2 * prompts, head), F32),
            pltpu.VMEM((prompts, head), F32),
            pltpu.VMEM((prompts, head), F32),
            pltpu.VMEM((n_tp, prompts, out_cols), F32),
            pltpu.VMEM((n_tp, prompts, out_cols), F32),
            dma((12,)),
            dma((max(n_tp, 7), prompts)),
            dma((n_tp, prompts)),
            dma((prompts,)),
            dma((prompts,)),
            dma((1,)),
            dma((1,)),
            dma((n_sp,)),
            dma((1,)),
            dma((n_tp,)),
            dma((n_tp,)),
        ],
        compiler_params=pltpu.CompilerParams(
            collective_id=0, has_side_effects=True, vmem_limit_bytes=64 * 2**20 - 900 * 2**10
        ),
    )(
        context,
        first,
        wk,
        wv,
        wq,
        wz,
        w_write.T,
        w_fade.T,
        speeds.reshape(1, heads),
        extra.reshape(prompts, 1, length),
        gain.reshape(1, head),
        w_exit,
    )
    return state[:, None, None].astype(BF), step.astype(BF)


def solution(mesh):
    placed = (
        P(None, "sp", "tp"),
        P(),
        P(None, "tp"),
        P(None, "tp"),
        P(None, "tp"),
        P(None, "tp"),
        P(),
        P(),
        P(),
        P(None, "sp", "tp"),
        P(),
        P("tp", None),
    )
    return jax.shard_map(
        functools.partial(body, mesh.shape["sp"], mesh.shape["tp"]),
        mesh=mesh,
        in_specs=placed,
        out_specs=(P(None, "sp", "tp", None, None), P(None, "tp")),
        check_vma=False,
    )
```
